32 devices in a mesh: dp: 2 (over x), kv: 8 (over z, y), tp: 2 (over core).
Axes of the slice: x: 2, y: 2, z: 4, core: 2. Of those that a mesh axis runs over, the one named last changes fastest.
Arguments:
- tokens: bfloat16 [48, 2048], P('dp', ('kv', 'tp')), may hold values from -21 to 21
- state: float32 [48, 8, 128, 128], P(('dp', 'kv'), 'tp'), may hold values from -3 to 3
- mix_gain: bfloat16 [2048], P(('kv', 'tp')), may hold values from 0.099609375 to 1.8984375
- w_query: bfloat16 [2048, 1024], P('kv', 'tp'), may hold values from -0.125 to 0.125
- w_key: bfloat16 [2048, 1024], P('kv', 'tp'), may hold values from -0.125 to 0.125
- w_value: bfloat16 [2048, 1024], P('kv', 'tp'), may hold values from -0.125 to 0.125
- w_beta: bfloat16 [2048, 8], P('kv', 'tp'), may hold values from -0.125 to 0.125
- w_decay: bfloat16 [2048, 8], P('kv', 'tp'), may hold values from -0.125 to 0.125
- decay_log: float32 [8], P('tp'), may hold values from -1.5 to 1
- head_gain: bfloat16 [128], replicated, may hold values from 0.099609375 to 1.8984375
- w_out: bfloat16 [1024, 2048], P('tp', 'kv'), may hold values from -0.1875 to 0.1875
- ff_gain: bfloat16 [2048], P(('kv', 'tp')), may hold values from 0.099609375 to 1.8984375
- w_up: bfloat16 [2048, 8192], P(None, ('kv', 'tp')), may hold values from -0.125 to 0.125
- w_down: bfloat16 [8192, 2048], P(('kv', 'tp')), may hold values from -0.09375 to 0.09375
Outputs:
- output: bfloat16 [48, 2048], P('dp', ('kv', 'tp'))
- new_state: float32 [48, 8, 128, 128], P(('dp', 'kv'), 'tp')
The draws below stay inside these ranges and needn't reach their ends.
All inputs are finite; a program needn't handle non-finite values.
Results may differ from the reference program's by a relative error of at most 0.013.
Values may be sent and summed in bfloat16 or wider, within the bound.
A program may use at most 64 MiB of HBM per device.

```python
import jax
import jax.numpy as jnp
from jax import lax

D = 2048
HEADS = 8
HEAD_DIM = 128
FF = 8192
BATCH = 48
KEYS = 1024
N_TP = 2


def draw_tokens(key, part):
    noise_key = jax.random.fold_in(key, 23)
    columns = jnp.arange(D, dtype=jnp.float32) / D
    entries = jnp.clip(jax.random.normal(noise_key, (BATCH, D), jnp.float32), -4.0, 4.0)
    values = entries * (4.0 ** columns)[None, :] * 0.5
    return values.astype(jnp.bfloat16)


def raised(result, own_key, source, target, parts, factor):
    owner, partner = [(jnp.arange(result.shape[axis_at]) // (result.shape[axis_at] // parts)).reshape([-1 if axis == axis_at else 1 for axis in range(result.ndim)]) for axis_at in (source, target)]
    chosen = jax.random.permutation(own_key, parts)[partner]
    strong = (owner == chosen) | (owner == (partner + parts // 2) % parts)
    return jnp.where(strong, factor * result, result)


def block_levels(rng, dims, split, low, largest):
    def one(position, shards_of):
        steps = jax.random.uniform(jax.random.fold_in(jax.random.fold_in(rng, 6), position), (shards_of,), jnp.float32, low / len(split), largest / len(split))
        return jnp.repeat(jnp.exp(steps), dims[position] // shards_of).reshape((-1,) + (1,) * (len(dims) - position - 1))

    loudness = one(*split[0])
    for cut in split[1:]:
        loudness = loudness * one(*cut)
    return loudness


def gaussian(key, shape, spread, bound, pieces=(), kind=jnp.bfloat16):
    factor_of = block_levels(key, shape, pieces, -0.22, 0.18) if pieces else 1.0
    values = jax.random.normal(key, shape, jnp.float32) * spread * factor_of
    return jnp.minimum(jnp.maximum(values, -bound), bound).astype(kind)


def gaussian_with(rng, extent, deviation, limit, split, heavy, kind=jnp.bfloat16):
    result = deviation * jax.random.normal(rng, extent, jnp.float32)
    if split:
        result = result * block_levels(rng, extent, split, -0.22, 0.18)
    return jnp.clip(raised(result, jax.random.fold_in(rng, 3), *heavy), -limit, limit).astype(kind)


def setup_inputs(seed: int = 0) -> dict:
    key_of = jax.random.split(jax.random.key(seed), 15)
    tokens = draw_tokens(jax.random.fold_in(key_of[14], 71), 0)
    state = gaussian(key_of[1], (BATCH, HEADS, HEAD_DIM, HEAD_DIM), 0.5, 3.0, ((0, 16), (1, 2)), jnp.float32)
    mix_gain = jnp.clip(1.0 + 0.18 * jax.random.normal(key_of[2], (D,), jnp.float32), 0.099609375, 1.8984375).astype(jnp.bfloat16)
    w_query = gaussian(key_of[3], (D, KEYS), D ** -0.5, 0.125, ((0, 8), (1, 2)))
    w_key = gaussian(key_of[4], (D, KEYS), D ** -0.5, 0.125, ((0, 8), (1, 2)))
    w_value = gaussian(key_of[5], (D, KEYS), D ** -0.5, 0.125, ((0, 8), (1, 2)))
    w_beta = gaussian(key_of[6], (D, HEADS), D ** -0.5, 0.125, ((0, 8), (1, 2)))
    w_decay = gaussian(key_of[7], (D, HEADS), D ** -0.5, 0.125, ((0, 8), (1, 2)))
    decay_log = jnp.clip(-1.5 + 2.5 * jax.random.uniform(key_of[8], (HEADS,), jnp.float32) ** block_levels(key_of[8], (HEADS,), ((0, 2),), -0.2, 0.2), -1.5, 1.0)
    head_gain = jnp.clip(1.0 + 0.18 * jax.random.normal(key_of[9], (HEAD_DIM,), jnp.float32), 0.099609375, 1.8984375).astype(jnp.bfloat16)
    w_out = gaussian(key_of[10], (KEYS, D), KEYS ** -0.5, 0.1875, ((0, 2), (1, 8)))
    ff_gain = jnp.clip(1.0 + 0.18 * jax.random.normal(key_of[11], (D,), jnp.float32), 0.099609375, 1.8984375).astype(jnp.bfloat16)
    w_up = gaussian(key_of[12], (D, FF), D ** -0.5, 0.125, ((1, 16),))
    w_down = gaussian_with(key_of[13], (FF, D), FF ** -0.5, 0.09375, ((0, 16),), (0, 1, 16, 2.0))
    return dict(tokens=tokens, state=state, mix_gain=mix_gain, w_query=w_query, w_key=w_key, w_value=w_value, w_beta=w_beta, w_decay=w_decay, decay_log=decay_log, head_gain=head_gain, w_out=w_out, ff_gain=ff_gain, w_up=w_up, w_down=w_down)


def reference(tokens, state, mix_gain, w_query, w_key, w_value, w_beta, w_decay, decay_log, head_gain, w_out, ff_gain, w_up, w_down):
    tokens_float = tokens.astype(jnp.float32)
    mean_square = lax.optimization_barrier(jnp.mean(tokens_float * tokens_float, axis=1, keepdims=True))
    scaled = (tokens_float * mix_gain.astype(jnp.float32)).astype(jnp.bfloat16)
    inverse = lax.rsqrt(mean_square + 1e-06)
    query = inverse * jnp.dot(scaled, w_query, preferred_element_type=jnp.float32)
    key_rows = inverse * jnp.dot(scaled, w_key, preferred_element_type=jnp.float32)
    value = inverse * jnp.dot(scaled, w_value, preferred_element_type=jnp.float32)
    beta = jax.nn.sigmoid(inverse * jnp.dot(scaled, w_beta, preferred_element_type=jnp.float32))
    decay = -jnp.exp(decay_log)[None, :] * jax.nn.softplus(inverse * jnp.dot(scaled, w_decay, preferred_element_type=jnp.float32))
    batch_rows = tokens.shape[0]
    query = query.reshape(batch_rows, HEADS, HEAD_DIM)
    key_rows = key_rows.reshape(batch_rows, HEADS, HEAD_DIM)
    value = value.reshape(batch_rows, HEADS, HEAD_DIM)
    qnorm = query * lax.rsqrt(lax.optimization_barrier(jnp.sum(query * query, axis=-1, keepdims=True)) + 1e-06)
    knorm = key_rows * lax.rsqrt(lax.optimization_barrier(jnp.sum(key_rows * key_rows, axis=-1, keepdims=True)) + 1e-06)
    kept = state * jnp.exp(decay)[:, :, None, None]
    predicted = lax.optimization_barrier(jnp.sum(kept * knorm[:, :, :, None], axis=2))
    new_state = kept + (beta[:, :, None] * knorm)[:, :, :, None] * (value - predicted)[:, :, None, :]
    heads = lax.optimization_barrier(jnp.sum(new_state * qnorm[:, :, :, None], axis=2)) / jnp.sqrt(jnp.float32(HEAD_DIM))
    normed = heads * lax.rsqrt(lax.optimization_barrier(jnp.mean(heads * heads, axis=-1, keepdims=True)) + 1e-06) * head_gain.astype(jnp.float32)
    normed = normed.astype(jnp.bfloat16).reshape(batch_rows, KEYS)
    half_width = KEYS // N_TP
    mixed = jnp.zeros((batch_rows, D), jnp.float32)
    for half_index in range(N_TP):
        lower = half_index * half_width
        product = jnp.dot(normed[:, lower:lower + half_width], w_out[lower:lower + half_width], preferred_element_type=jnp.float32)
        mixed = mixed + product.astype(jnp.bfloat16).astype(jnp.float32)
    resid = (tokens_float + mixed).astype(jnp.bfloat16)
    resid_float = resid.astype(jnp.float32)
    mean_square2 = lax.optimization_barrier(jnp.mean(resid_float * resid_float, axis=1, keepdims=True))
    scaled2 = (resid_float * ff_gain.astype(jnp.float32)).astype(jnp.bfloat16)
    up_rows = jnp.dot(scaled2, w_up, preferred_element_type=jnp.float32) * lax.rsqrt(mean_square2 + 1e-06)
    act = jnp.square(jax.nn.relu(up_rows)).astype(jnp.bfloat16)
    output = (resid_float + jnp.dot(act, w_down, preferred_element_type=jnp.float32)).astype(jnp.bfloat16)
    return (output, new_state)
```

```python
import functools

import jax
import jax.numpy as jnp
from jax import lax
from jax.experimental import pallas as pl
from jax.experimental.pallas import tpu as pltpu
from jax.sharding import PartitionSpec as P

D = 2048


def local(
    tokens,
    state,
    mix_gain,
    w_query,
    w_key,
    w_value,
    w_beta,
    w_decay,
    decay_log,
    head_gain,
    w_out,
    ff_gain,
    w_up,
    w_down,
):
    seq_count = state.shape[0]
    heads_local = state.shape[1]
    head_size = state.shape[2]
    tokens_wide, gain_wide = (
        lax.all_gather(tokens, "tp", axis=1, tiled=True),
        lax.all_gather(mix_gain[None, :], "tp", axis=1, tiled=True),
    )
    wide_float = tokens_wide.astype(jnp.float32)
    scaled = (wide_float * gain_wide.astype(jnp.float32)).astype(jnp.bfloat16)
    query_part = jnp.dot(scaled, w_query, preferred_element_type=jnp.float32)
    key_part = jnp.dot(scaled, w_key, preferred_element_type=jnp.float32)
    value_part = jnp.dot(scaled, w_value, preferred_element_type=jnp.float32)
    gate_part = jnp.concatenate(
        [
            jnp.dot(scaled, w_beta, preferred_element_type=jnp.float32),
            jnp.dot(scaled, w_decay, preferred_element_type=jnp.float32),
        ],
        axis=1,
    )
    square_part = jnp.sum(wide_float * wide_float, axis=1)
    query_sum, key_sum, value_sum, gate_sum, square_sum = (
        lax.psum_scatter(query_part, "kv", scatter_dimension=0, tiled=True),
        lax.psum_scatter(key_part, "kv", scatter_dimension=0, tiled=True),
        lax.psum_scatter(value_part, "kv", scatter_dimension=0, tiled=True),
        lax.psum_scatter(gate_part, "kv", scatter_dimension=0, tiled=True),
        lax.psum_scatter(square_part, "kv", scatter_dimension=0, tiled=True),
    )
    inverse = lax.rsqrt(square_sum / D + 1e-06)[:, None]
    query = (inverse * query_sum).reshape(seq_count, heads_local, head_size)
    key_rows = (inverse * key_sum).reshape(seq_count, heads_local, head_size)
    value = (inverse * value_sum).reshape(seq_count, heads_local, head_size)
    gates = inverse * gate_sum
    beta = jax.nn.sigmoid(gates[:, :heads_local])
    decay = -jnp.exp(decay_log)[None, :] * jax.nn.softplus(gates[:, heads_local:])
    qnorm = query * lax.rsqrt(jnp.sum(query * query, axis=-1, keepdims=True) + 1e-06)
    knorm = key_rows * lax.rsqrt(jnp.sum(key_rows * key_rows, axis=-1, keepdims=True) + 1e-06)
    kept = state * jnp.exp(decay)[:, :, None, None]
    predicted = jnp.sum(kept * knorm[:, :, :, None], axis=2)
    new_state = (
        kept + (beta[:, :, None] * knorm)[:, :, :, None] * (value - predicted)[:, :, None, :]
    )
    heads = jnp.sum(new_state * qnorm[:, :, :, None], axis=2) / jnp.sqrt(jnp.float32(head_size))
    normed = (
        heads
        * lax.rsqrt(jnp.mean(heads * heads, axis=-1, keepdims=True) + 1e-06)
        * head_gain.astype(jnp.float32)
    )
    normed = normed.astype(jnp.bfloat16).reshape(seq_count, heads_local * head_size)
    partial_mix = jnp.dot(
        lax.all_gather(normed, "kv", axis=0, tiled=True), w_out, preferred_element_type=jnp.float32
    )
    mixed = lax.psum_scatter(
        partial_mix.astype(jnp.bfloat16), "tp", scatter_dimension=1, tiled=True
    ).astype(jnp.float32)
    resid = (tokens.astype(jnp.float32) + mixed).astype(jnp.bfloat16)
    resid_float = resid.astype(jnp.float32)
    whole_rows = lax.all_gather(resid, ("kv", "tp"), axis=1, tiled=True)
    whole_gain = lax.all_gather(ff_gain[None, :], ("kv", "tp"), axis=1, tiled=True)
    whole_float = whole_rows.astype(jnp.float32)
    inverse2 = lax.rsqrt(jnp.mean(whole_float * whole_float, axis=1, keepdims=True) + 1e-06)
    scaled2 = (whole_float * whole_gain.astype(jnp.float32)).astype(jnp.bfloat16)
    up_rows = jnp.dot(scaled2, w_up, preferred_element_type=jnp.float32) * inverse2
    act = jnp.square(jax.nn.relu(up_rows)).astype(jnp.bfloat16)
    summed = lax.psum_scatter(
        lax.dot_general(w_down, act, (((0,), (1,)), ((), ())), preferred_element_type=jnp.float32),
        ("kv", "tp"),
        scatter_dimension=0,
        tiled=True,
    )
    results = (resid_float + summed.T).astype(jnp.bfloat16)
    return (results, new_state)


LANES = 128
MESH = pl.DeviceIdType.MESH
F32 = jnp.float32
BF16 = jnp.bfloat16


def fused_kernel(
    n_kv,
    n_tp,
    tok_hbm, state_hbm, mg_hbm, wq_hbm, wk_hbm, wv_hbm, wb_hbm, wd_hbm, dl_hbm, hg_hbm,
    wo_hbm, fg_hbm, wup_hbm, wdn_hbm,
    out_ref, ns_hbm,
    tok, state, mg, wqkv, wb, wd, dl, hg, wo, fg, wup, wdn,
    x1_send, x1_recv, parts, rows, x2_send, x2_recv,
    x3_send, x3_recv, heads_f32, left,
    x5_send, x5_recv, x6_send, x6_recv,
    load_sem, store_sem, x1_sems, wo_sems, s2, r2, s3, r3, s5, r5, s6, r6,
):
    kv = lax.axis_index("kv")
    tp = lax.axis_index("tp")
    other = 1 - tp
    n_dev = n_kv * n_tp
    me = kv * n_tp + tp
    batch = tok.shape[0]
    seqs, n_heads, size = state.shape[0], state.shape[1], state.shape[2]
    wide = n_heads * size
    d_model = n_dev * LANES
    items = n_heads * seqs
    stride2 = x2_send.shape[1]
    stride3 = x3_recv.shape[1]

    def place(device):
        return {"kv": device // n_tp, "tp": lax.rem(device, n_tp)}

    loads = [
        (tok_hbm, tok), (mg_hbm, mg),
        (wq_hbm, wqkv.at[:, 0:wide]),
        (wk_hbm, wqkv.at[:, wide:2 * wide]),
        (wv_hbm, wqkv.at[:, 2 * wide:3 * wide]),
        (wb_hbm, wb), (wd_hbm, wd), (dl_hbm, dl), (hg_hbm, hg), (fg_hbm, fg),
        (wo_hbm.at[:, pl.ds(pl.multiple_of(tp * LANES, LANES), LANES)], wo.at[tp]),
        (state_hbm, state), (wup_hbm, wup), (wdn_hbm, wdn),
    ]
    copies = [
        pltpu.make_async_copy(a, b, load_sem.at[i]) for i, (a, b) in enumerate(loads)
    ]
    for copy in copies:
        copy.start()

    barrier = pltpu.get_barrier_semaphore()
    for step in range(1, n_dev):
        pl.semaphore_signal(
            barrier, inc=1, device_id=place(lax.rem(me + step, n_dev)), device_id_type=MESH
        )
    rows[...] = jnp.zeros_like(rows)
    copies[0].wait()
    copies[1].wait()
    own = tok[...].astype(F32)
    own_gain = mg[...].astype(F32)
    x1_send[0:batch, :] = tok[...]
    x1_send[batch:, :] = jnp.broadcast_to(own_gain, (x1_send.shape[0] - batch, LANES)).astype(BF16)
    pl.semaphore_wait(barrier, n_dev - 1)

    x1 = pltpu.make_async_remote_copy(
        x1_send, x1_recv, x1_sems.at[0], x1_sems.at[1], device_id={"tp": other}, device_id_type=MESH
    )
    x1.start()
    wo_copy = pltpu.make_async_remote_copy(
        wo_hbm.at[:, pl.ds(pl.multiple_of(other * LANES, LANES), LANES)],
        wo.at[tp], wo_sems.at[0], wo_sems.at[1], device_id={"tp": other}, device_id_type=MESH,
    )
    wo_copy.start()
    for copy in copies[2:7]:
        copy.wait()
    gate_w = jnp.concatenate(
        [
            wb[...].astype(F32), wd[...].astype(F32),
            jnp.zeros((wb.shape[0], LANES - 2 * n_heads), F32),
        ],
        axis=1,
    ).astype(BF16)
    own_scaled = own * own_gain
    x1.wait()
    far = x1_recv[0:batch, :].astype(F32)
    far_scaled = far * x1_recv[batch:, :].astype(F32)[0:1, :]
    first = tp == 0
    scaled = jnp.concatenate(
        [jnp.where(first, own_scaled, far_scaled), jnp.where(first, far_scaled, own_scaled)], axis=1
    ).astype(BF16)
    squares = jnp.sum(own * own + far * far, axis=1, keepdims=True)
    gates = jnp.dot(scaled, gate_w, preferred_element_type=F32)
    lane = lax.broadcasted_iota(jnp.int32, gates.shape, 1)
    gates = jnp.where(lane == 2 * n_heads, squares, gates)
    gates_hi = gates.astype(BF16).astype(F32)
    chunks = 3 * n_heads
    product = jnp.dot(scaled, wqkv[...], preferred_element_type=F32)
    for c in range(chunks):
        parts[c] = product[:, c * LANES:(c + 1) * LANES]
    parts[chunks] = gates_hi
    parts[chunks + 1] = gates - gates_hi
    for c in range(chunks + 2):
        for s in range(seqs):
            rows[pl.ds(c * seqs + s, n_kv, stride=stride2), :] = parts[
                c, pl.ds(s, n_kv, stride=seqs), :
            ]
    x2_send[...] = rows[...].reshape(x2_send.shape).astype(BF16)

    sent2 = []
    for step in range(1, n_kv):
        peer = lax.rem(kv + step, n_kv)
        copy = pltpu.make_async_remote_copy(
            x2_send.at[peer], x2_recv.at[kv], s2.at[step], r2.at[kv],
            device_id={"kv": peer}, device_id_type=MESH,
        )
        copy.start()
        sent2.append(copy)
    x2_recv[kv] = x2_send[kv]
    for copy in copies[7:12]:
        copy.wait()
    for step in range(1, n_kv):
        source = lax.rem(kv + step, n_kv)
        pltpu.make_async_remote_copy(
            x2_send.at[source], x2_recv.at[source], s2.at[step], r2.at[source],
            device_id={"kv": source}, device_id_type=MESH,
        ).wait_recv()
    total = x2_recv[0].astype(F32)
    for k in range(1, n_kv):
        total = total + x2_recv[k].astype(F32)

    g0 = 3 * items
    gate = total[g0:g0 + seqs, :] + total[g0 + seqs:g0 + 2 * seqs, :]
    inverse = lax.rsqrt(gate[:, 2 * n_heads:2 * n_heads + 1] / d_model + 1e-06)
    gate = gate * inverse
    beta = jax.nn.sigmoid(gate[:, 0:n_heads])
    decay = jnp.exp(-jnp.exp(dl[...]) * jax.nn.softplus(gate[:, n_heads:2 * n_heads]))
    inv_col = jnp.concatenate([inverse] * n_heads, axis=0)
    query = total[0:items, :] * inv_col
    key_rows = total[items:2 * items, :] * inv_col
    value = total[2 * items:3 * items, :] * inv_col
    qnorm = query * lax.rsqrt(jnp.sum(query * query, axis=1, keepdims=True) + 1e-06)
    knorm = key_rows * lax.rsqrt(jnp.sum(key_rows * key_rows, axis=1, keepdims=True) + 1e-06)
    fill = jnp.zeros((-items % 8, LANES), F32)
    cols = jnp.transpose(jnp.concatenate([qnorm, fill, knorm, fill], axis=0))
    k0 = items + fill.shape[0]
    outs = []
    for h in range(n_heads):
        for s in range(seqs):
            i = h * seqs + s
            kept = state[s, h] * decay[s:s + 1, h:h + 1]
            k_col = cols[:, k0 + i:k0 + i + 1]
            q_col = cols[:, i:i + 1]
            predicted = jnp.sum(kept * k_col, axis=0, keepdims=True)
            delta = beta[s:s + 1, h:h + 1] * (value[i:i + 1, :] - predicted)
            new = kept + k_col * delta
            state[s, h] = new
            outs.append(jnp.sum(new * q_col, axis=0, keepdims=True))
    heads = jnp.concatenate(outs, axis=0) / jnp.sqrt(F32(size))
    normed = (
        heads * lax.rsqrt(jnp.mean(heads * heads, axis=1, keepdims=True) + 1e-06)
        * hg[...].astype(F32)
    )
    x3_send[...] = jnp.concatenate(
        [normed, jnp.broadcast_to(fg[...].astype(F32), (stride3 - items, LANES))], axis=0
    ).astype(BF16)

    sent3 = []
    for step in range(1, n_dev):
        copy = pltpu.make_async_remote_copy(
            x3_send, x3_recv.at[me], s3.at[step], r3.at[me],
            device_id=place(lax.rem(me + step, n_dev)), device_id_type=MESH,
        )
        copy.start()
        sent3.append(copy)
    ns_copy = pltpu.make_async_copy(state, ns_hbm, store_sem)
    ns_copy.start()
    x3_recv[me] = x3_send[...]
    wo_copy.wait()
    for step in range(1, n_dev):
        source = lax.rem(me + step, n_dev)
        pltpu.make_async_remote_copy(
            x3_send, x3_recv.at[source], s3.at[step], r3.at[source],
            device_id=place(source), device_id_type=MESH,
        ).wait_recv()
    heads_f32[...] = x3_recv[...].astype(F32).reshape(heads_f32.shape)
    for t in range(n_tp):
        for h in range(n_heads):
            for s in range(seqs):
                left[t * n_heads + h, pl.ds(s, n_kv, stride=seqs), :] = heads_f32[
                    pl.ds(t * stride3 + h * seqs + s, n_kv, stride=n_tp * stride3), :
                ]
    mixed = None
    for t in range(n_tp):
        lhs = jnp.concatenate(
            [left[t * n_heads + h].astype(BF16) for h in range(n_heads)], axis=1
        )
        half = jnp.dot(lhs, wo[t], preferred_element_type=F32).astype(BF16).astype(F32)
        mixed = half if mixed is None else mixed + half
    resid = (own + mixed).astype(BF16)
    x5_send[...] = resid

    sent5 = []
    for step in range(1, n_dev):
        copy = pltpu.make_async_remote_copy(
            x5_send, x5_recv.at[me], s5.at[step], r5.at[me],
            device_id=place(lax.rem(me + step, n_dev)), device_id_type=MESH,
        )
        copy.start()
        sent5.append(copy)
    x5_recv[me] = resid
    copies[12].wait()

    def arrived5(source):
        pltpu.make_async_remote_copy(
            x5_send, x5_recv.at[source], s5.at[0], r5.at[source],
            device_id=place(source), device_id_type=MESH,
        ).wait_recv()

    up_rows = None
    square2 = None
    for step in range(n_kv):
        chip = lax.rem(kv + step, n_kv)
        if step == 0:
            arrived5(kv * n_tp + other)
        else:
            for t in range(n_tp):
                arrived5(chip * n_tp + t)
        blocks = []
        for t in range(n_tp):
            block = x5_recv[chip * n_tp + t].astype(F32)
            gain = x3_recv[chip * n_tp + t].astype(F32)[items:items + 1, :]
            square2 = block * block if square2 is None else square2 + block * block
            blocks.append((block * gain).astype(BF16))
        deep = n_tp * LANES
        term = jnp.dot(
            jnp.concatenate(blocks, axis=1),
            wup[pl.ds(pl.multiple_of(chip * deep, deep), deep), :],
            preferred_element_type=F32,
        )
        up_rows = term if up_rows is None else up_rows + term
    inverse2 = lax.rsqrt(jnp.sum(square2, axis=1, keepdims=True) / d_model + 1e-06)
    act = jnp.square(jnp.maximum(up_rows * inverse2, 0.0)).astype(BF16)

    copies[13].wait()
    sent6 = []
    own_sum = None
    for step in range(1, n_kv + 1):
        chip = lax.rem(kv + step, n_kv)
        deep = n_tp * LANES
        piece = jnp.dot(
            act, wdn[:, pl.ds(pl.multiple_of(chip * deep, deep), deep)], preferred_element_type=F32
        )
        for t in range(n_tp):
            x6_send[chip * n_tp + t] = piece[:, t * LANES:(t + 1) * LANES].astype(BF16)
        if step < n_kv:
            for t in range(n_tp):
                copy = pltpu.make_async_remote_copy(
                    x6_send.at[chip * n_tp + t], x6_recv.at[me],
                    s6.at[step * n_tp + t], r6.at[me],
                    device_id={"kv": chip, "tp": t}, device_id_type=MESH,
                )
                copy.start()
                sent6.append(copy)
        else:
            copy = pltpu.make_async_remote_copy(
                x6_send.at[chip * n_tp + other], x6_recv.at[me],
                s6.at[0], r6.at[me], device_id={"tp": other}, device_id_type=MESH,
            )
            copy.start()
            sent6.append(copy)
            own_sum = jnp.where(first, piece[:, 0:LANES], piece[:, LANES:2 * LANES])
    summed = resid.astype(F32) + own_sum
    for step in range(1, n_dev):
        source = lax.rem(me + step, n_dev)
        pltpu.make_async_remote_copy(
            x6_send.at[source], x6_recv.at[source], s6.at[0], r6.at[source],
            device_id=place(source), device_id_type=MESH,
        ).wait_recv()
        summed = summed + x6_recv[source].astype(F32)
    out_ref[...] = summed.astype(BF16)
    for copy in sent2 + sent3 + sent5 + sent6:
        copy.wait_send()
    ns_copy.wait()


def fused(n_kv, n_tp, *args):
    (tokens, state, mix_gain, w_query, w_key, w_value, w_beta, w_decay, decay_log, head_gain,
     w_out, ff_gain, w_up, w_down) = args
    batch = tokens.shape[0]
    seqs, n_heads = state.shape[:2]
    items = seqs * n_heads
    n_dev = n_kv * n_tp
    chunks = 3 * n_heads + 2
    stride2 = -(-chunks * seqs // 16) * 16
    stride3 = -(-(items + 1) // 16) * 16
    wide = w_query.shape[1]
    operands = (
        tokens, state, mix_gain[None, :], w_query, w_key, w_value, w_beta, w_decay,
        decay_log[None, :], head_gain[None, :], w_out, ff_gain[None, :], w_up, w_down,
    )
    dma = pltpu.SemaphoreType.DMA
    vmem = pltpu.VMEM
    scratch = [
        vmem(tokens.shape, BF16), vmem(state.shape, F32), vmem((1, LANES), BF16),
        vmem((w_query.shape[0], 3 * wide), BF16), vmem(w_beta.shape, BF16),
        vmem(w_decay.shape, BF16), vmem((1, n_heads), F32), vmem((1, LANES), BF16),
        vmem((n_tp, w_out.shape[0], LANES), BF16), vmem((1, LANES), BF16),
        vmem(w_up.shape, BF16), vmem(w_down.shape, BF16),
        vmem((batch + 8, LANES), BF16), vmem((batch + 8, LANES), BF16),
        vmem((chunks, batch, LANES), F32), vmem((n_kv * stride2, LANES), F32),
        vmem((n_kv, stride2, LANES), BF16), vmem((n_kv, stride2, LANES), BF16),
        vmem((stride3, LANES), BF16), vmem((n_dev, stride3, LANES), BF16),
        vmem((n_dev * stride3, LANES), F32), vmem((n_tp * n_heads, batch, LANES), F32),
        vmem((batch, LANES), BF16), vmem((n_dev, batch, LANES), BF16),
        vmem((n_dev, batch, LANES), BF16), vmem((n_dev, batch, LANES), BF16),
        dma((14,)), dma, dma((2,)), dma((2,)),
        dma((n_kv,)), dma((n_kv,)), dma((n_dev,)), dma((n_dev,)),
        dma((n_dev,)), dma((n_dev,)), dma((n_dev,)), dma((n_dev,)),
    ]
    return pl.pallas_call(
        functools.partial(fused_kernel, n_kv, n_tp),
        out_shape=(
            jax.ShapeDtypeStruct(tokens.shape, BF16), jax.ShapeDtypeStruct(state.shape, F32),
        ),
        in_specs=[pl.BlockSpec(memory_space=pl.ANY)] * len(operands),
        out_specs=(pl.BlockSpec(memory_space=pltpu.VMEM), pl.BlockSpec(memory_space=pl.ANY)),
        scratch_shapes=scratch,
        compiler_params=pltpu.CompilerParams(
            collective_id=0, has_side_effects=True, vmem_limit_bytes=60 * 1024 * 1024
        ),
    )(*operands)


def block_of(n_kv, n_tp, *args):
    tokens, state = args[:2]
    fits = (
        tokens.shape[1] == LANES and n_kv == 8 and n_tp == 2
        and state.shape[3] == LANES and tokens.shape[0] % 8 == 0
    )
    return fused(n_kv, n_tp, *args) if fits else local(*args)


def solution(mesh):
    placed = (
        P("dp", ("kv", "tp")),
        P(("dp", "kv"), "tp", None, None),
        P(("kv", "tp")),
        P("kv", "tp"),
        P("kv", "tp"),
        P("kv", "tp"),
        P("kv", "tp"),
        P("kv", "tp"),
        P("tp"),
        P(),
        P("tp", "kv"),
        P(("kv", "tp")),
        P(None, ("kv", "tp")),
        P(("kv", "tp"), None),
    )
    return jax.shard_map(
        functools.partial(block_of, mesh.shape["kv"], mesh.shape["tp"]),
        mesh=mesh,
        in_specs=placed,
        out_specs=(P("dp", ("kv", "tp")), P(("dp", "kv"), "tp", None, None)),
        check_vma=False,
    )
```

```python
import functools

import jax
import jax.numpy as jnp
from jax import lax
from jax.experimental import pallas as pl
from jax.experimental.pallas import tpu as pltpu
from jax.sharding import PartitionSpec as P

D = 2048


def local(
    tokens,
    state,
    mix_gain,
    w_query,
    w_key,
    w_value,
    w_beta,
    w_decay,
    decay_log,
    head_gain,
    w_out,
    ff_gain,
    w_up,
    w_down,
):
    seq_count = state.shape[0]
    heads_local = state.shape[1]
    head_size = state.shape[2]
    tokens_wide, gain_wide = (
        lax.all_gather(tokens, "tp", axis=1, tiled=True),
        lax.all_gather(mix_gain[None, :], "tp", axis=1, tiled=True),
    )
    wide_float = tokens_wide.astype(jnp.float32)
    scaled = (wide_float * gain_wide.astype(jnp.float32)).astype(jnp.bfloat16)
    query_part = jnp.dot(scaled, w_query, preferred_element_type=jnp.float32)
    key_part = jnp.dot(scaled, w_key, preferred_element_type=jnp.float32)
    value_part = jnp.dot(scaled, w_value, preferred_element_type=jnp.float32)
    gate_part = jnp.concatenate(
        [
            jnp.dot(scaled, w_beta, preferred_element_type=jnp.float32),
            jnp.dot(scaled, w_decay, preferred_element_type=jnp.float32),
        ],
        axis=1,
    )
    square_part = jnp.sum(wide_float * wide_float, axis=1)
    query_sum, key_sum, value_sum, gate_sum, square_sum = (
        lax.psum_scatter(query_part, "kv", scatter_dimension=0, tiled=True),
        lax.psum_scatter(key_part, "kv", scatter_dimension=0, tiled=True),
        lax.psum_scatter(value_part, "kv", scatter_dimension=0, tiled=True),
        lax.psum_scatter(gate_part, "kv", scatter_dimension=0, tiled=True),
        lax.psum_scatter(square_part, "kv", scatter_dimension=0, tiled=True),
    )
    inverse = lax.rsqrt(square_sum / D + 1e-06)[:, None]
    query = (inverse * query_sum).reshape(seq_count, heads_local, head_size)
    key_rows = (inverse * key_sum).reshape(seq_count, heads_local, head_size)
    value = (inverse * value_sum).reshape(seq_count, heads_local, head_size)
    gates = inverse * gate_sum
    beta = jax.nn.sigmoid(gates[:, :heads_local])
    decay = -jnp.exp(decay_log)[None, :] * jax.nn.softplus(gates[:, heads_local:])
    qnorm = query * lax.rsqrt(jnp.sum(query * query, axis=-1, keepdims=True) + 1e-06)
    knorm = key_rows * lax.rsqrt(jnp.sum(key_rows * key_rows, axis=-1, keepdims=True) + 1e-06)
    kept = state * jnp.exp(decay)[:, :, None, None]
    predicted = jnp.sum(kept * knorm[:, :, :, None], axis=2)
    new_state = (
        kept + (beta[:, :, None] * knorm)[:, :, :, None] * (value - predicted)[:, :, None, :]
    )
    heads = jnp.sum(new_state * qnorm[:, :, :, None], axis=2) / jnp.sqrt(jnp.float32(head_size))
    normed = (
        heads
        * lax.rsqrt(jnp.mean(heads * heads, axis=-1, keepdims=True) + 1e-06)
        * head_gain.astype(jnp.float32)
    )
    normed = normed.astype(jnp.bfloat16).reshape(seq_count, heads_local * head_size)
    partial_mix = jnp.dot(
        lax.all_gather(normed, "kv", axis=0, tiled=True), w_out, preferred_element_type=jnp.float32
    )
    mixed = lax.psum_scatter(
        partial_mix.astype(jnp.bfloat16), "tp", scatter_dimension=1, tiled=True
    ).astype(jnp.float32)
    resid = (tokens.astype(jnp.float32) + mixed).astype(jnp.bfloat16)
    resid_float = resid.astype(jnp.float32)
    whole_rows = lax.all_gather(resid, ("kv", "tp"), axis=1, tiled=True)
    whole_gain = lax.all_gather(ff_gain[None, :], ("kv", "tp"), axis=1, tiled=True)
    whole_float = whole_rows.astype(jnp.float32)
    inverse2 = lax.rsqrt(jnp.mean(whole_float * whole_float, axis=1, keepdims=True) + 1e-06)
    scaled2 = (whole_float * whole_gain.astype(jnp.float32)).astype(jnp.bfloat16)
    up_rows = jnp.dot(scaled2, w_up, preferred_element_type=jnp.float32) * inverse2
    act = jnp.square(jax.nn.relu(up_rows)).astype(jnp.bfloat16)
    summed = lax.psum_scatter(
        lax.dot_general(w_down, act, (((0,), (1,)), ((), ())), preferred_element_type=jnp.float32),
        ("kv", "tp"),
        scatter_dimension=0,
        tiled=True,
    )
    results = (resid_float + summed.T).astype(jnp.bfloat16)
    return (results, new_state)


LANES = 128
MESH = pl.DeviceIdType.MESH
F32 = jnp.float32
BF16 = jnp.bfloat16


def fused_kernel(
    n_kv,
    n_tp,
    tok_hbm, state_hbm, mg_hbm, wq_hbm, wk_hbm, wv_hbm, wb_hbm, wd_hbm, dl_hbm, hg_hbm,
    wo_hbm, fg_hbm, wup_hbm, wdn_hbm,
    out_ref, state,
    tok, mg, wqkv, wb, wd, dl, hg, wo, fg, wup, wdn,
    x1_send, x1_recv, parts, rows, x2_send, x2_recv,
    x3_send, x3_recv, heads_f32, left,
    x5_send, x5_recv, x6_send, x6_recv,
    load_sem, x1_sems, wo_sems, s2, r2, s3, r3, s5, r5, s6, r6,
):
    kv = lax.axis_index("kv")
    tp = lax.axis_index("tp")
    other = 1 - tp
    n_dev = n_kv * n_tp
    me = kv * n_tp + tp
    batch = tok.shape[0]
    seqs, n_heads, size = state.shape[0], state.shape[1], state.shape[2]
    wide = n_heads * size
    d_model = n_dev * LANES
    items = n_heads * seqs
    stride2 = x2_send.shape[1]
    stride3 = x3_recv.shape[1]

    far_first = sorted(range(1, n_kv), key=lambda step: -min(step, n_kv - step))
    far_devices = [step * n_tp + t for step in far_first for t in range(n_tp)]
    partner = kv * n_tp + other

    def place(device):
        return {"kv": device // n_tp, "tp": lax.rem(device, n_tp)}

    loads = [
        (tok_hbm, tok), (mg_hbm, mg),
        (wq_hbm, wqkv.at[:, 0:wide]),
        (wk_hbm, wqkv.at[:, wide:2 * wide]),
        (wv_hbm, wqkv.at[:, 2 * wide:3 * wide]),
        (wb_hbm, wb), (wd_hbm, wd), (dl_hbm, dl), (hg_hbm, hg), (fg_hbm, fg),
        (wo_hbm.at[:, pl.ds(pl.multiple_of(tp * LANES, LANES), LANES)], wo.at[tp]),
        (state_hbm, state), (wup_hbm, wup), (wdn_hbm, wdn),
    ]
    copies = [
        pltpu.make_async_copy(a, b, load_sem.at[i]) for i, (a, b) in enumerate(loads)
    ]
    for copy in copies:
        copy.start()

    barrier = pltpu.get_barrier_semaphore()
    for step in range(1, n_dev):
        pl.semaphore_signal(
            barrier, inc=1, device_id=place(lax.rem(me + step, n_dev)), device_id_type=MESH
        )
    rows[...] = jnp.zeros_like(rows)
    copies[0].wait()
    copies[1].wait()
    own = tok[...].astype(F32)
    own_gain = mg[...].astype(F32)
    x1_send[0:batch, :] = tok[...]
    x1_send[batch:, :] = jnp.broadcast_to(own_gain, (x1_send.shape[0] - batch, LANES)).astype(BF16)
    pl.semaphore_wait(barrier, n_dev - 1)

    x1 = pltpu.make_async_remote_copy(
        x1_send, x1_recv, x1_sems.at[0], x1_sems.at[1], device_id={"tp": other}, device_id_type=MESH
    )
    x1.start()
    wo_copy = pltpu.make_async_remote_copy(
        wo_hbm.at[:, pl.ds(pl.multiple_of(other * LANES, LANES), LANES)],
        wo.at[tp], wo_sems.at[0], wo_sems.at[1], device_id={"tp": other}, device_id_type=MESH,
    )
    wo_copy.start()
    for copy in copies[2:7]:
        copy.wait()
    gate_w = jnp.concatenate(
        [
            wb[...].astype(F32), wd[...].astype(F32),
            jnp.zeros((LANES - 2 * n_heads, wb.shape[1]), F32),
        ],
        axis=0,
    ).astype(BF16)
    own_scaled = own * own_gain
    x1.wait()
    far = x1_recv[0:batch, :].astype(F32)
    far_scaled = far * x1_recv[batch:, :].astype(F32)[0:1, :]
    first = tp == 0
    scaled = jnp.concatenate(
        [jnp.where(first, own_scaled, far_scaled), jnp.where(first, far_scaled, own_scaled)], axis=1
    ).astype(BF16)
    squares = jnp.sum(own * own + far * far, axis=1, keepdims=True)
    gates = lax.dot_general(
        scaled, gate_w, (((1,), (1,)), ((), ())), preferred_element_type=F32
    )
    lane = lax.broadcasted_iota(jnp.int32, gates.shape, 1)
    gates = jnp.where(lane == 2 * n_heads, squares, gates)
    gates_hi = gates.astype(BF16).astype(F32)
    chunks = 3 * n_heads
    product = jnp.dot(scaled, wqkv[...], preferred_element_type=F32)
    for c in range(chunks):
        parts[c] = product[:, c * LANES:(c + 1) * LANES]
    parts[chunks] = gates_hi
    parts[chunks + 1] = gates - gates_hi
    for c in range(chunks + 2):
        for s in range(seqs):
            rows[pl.ds(c * seqs + s, n_kv, stride=stride2), :] = parts[
                c, pl.ds(s, n_kv, stride=seqs), :
            ]
    x2_send[...] = rows[...].reshape(x2_send.shape).astype(BF16)

    sent2 = []
    for step in far_first:
        peer = lax.rem(kv + step, n_kv)
        copy = pltpu.make_async_remote_copy(
            x2_send.at[peer], x2_recv.at[kv], s2.at[step], r2.at[kv],
            device_id={"kv": peer}, device_id_type=MESH,
        )
        copy.start()
        sent2.append(copy)
    x2_recv[kv] = x2_send[kv]
    for copy in copies[7:12]:
        copy.wait()
    for step in range(1, n_kv):
        source = lax.rem(kv + step, n_kv)
        pltpu.make_async_remote_copy(
            x2_send.at[source], x2_recv.at[source], s2.at[step], r2.at[source],
            device_id={"kv": source}, device_id_type=MESH,
        ).wait_recv()
    total = x2_recv[0].astype(F32)
    for k in range(1, n_kv):
        total = total + x2_recv[k].astype(F32)

    g0 = 3 * items
    gate = total[g0:g0 + seqs, :] + total[g0 + seqs:g0 + 2 * seqs, :]
    inverse = lax.rsqrt(gate[:, 2 * n_heads:2 * n_heads + 1] / d_model + 1e-06)
    gate = gate * inverse
    beta = jax.nn.sigmoid(gate[:, 0:n_heads])
    decay = jnp.exp(-jnp.exp(dl[...]) * jax.nn.softplus(gate[:, n_heads:2 * n_heads]))
    inv_col = jnp.concatenate([inverse] * n_heads, axis=0)
    query = total[0:items, :] * inv_col
    key_rows = total[items:2 * items, :] * inv_col
    value = total[2 * items:3 * items, :] * inv_col
    qnorm = query * lax.rsqrt(jnp.sum(query * query, axis=1, keepdims=True) + 1e-06)
    knorm = key_rows * lax.rsqrt(jnp.sum(key_rows * key_rows, axis=1, keepdims=True) + 1e-06)
    fill = jnp.zeros((-items % 8, LANES), F32)
    cols = jnp.transpose(jnp.concatenate([qnorm, fill, knorm, fill], axis=0))
    k0 = items + fill.shape[0]
    along_k, along_q = [], []
    for h in range(n_heads):
        for s in range(seqs):
            i = h * seqs + s
            before = state[s, h]
            along_k.append(jnp.sum(before * cols[:, k0 + i:k0 + i + 1], axis=0, keepdims=True))
            along_q.append(jnp.sum(before * cols[:, i:i + 1], axis=0, keepdims=True))
    beta_col = jnp.concatenate([beta[:, h:h + 1] for h in range(n_heads)], axis=0)
    decay_col = jnp.concatenate([decay[:, h:h + 1] for h in range(n_heads)], axis=0)
    delta = beta_col * (value - decay_col * jnp.concatenate(along_k, axis=0))
    heads = (
        decay_col * jnp.concatenate(along_q, axis=0)
        + jnp.sum(qnorm * knorm, axis=1, keepdims=True) * delta
    ) / jnp.sqrt(F32(size))
    normed = (
        heads * lax.rsqrt(jnp.mean(heads * heads, axis=1, keepdims=True) + 1e-06)
        * hg[...].astype(F32)
    )
    x3_send[...] = jnp.concatenate(
        [normed, jnp.broadcast_to(fg[...].astype(F32), (stride3 - items, LANES))], axis=0
    ).astype(BF16)

    sent3 = []
    for step in far_devices + [0]:
        peer = lax.rem(kv * n_tp + step, n_dev) if step else partner
        copy = pltpu.make_async_remote_copy(
            x3_send, x3_recv.at[me], s3.at[step], r3.at[me],
            device_id=place(peer), device_id_type=MESH,
        )
        copy.start()
        sent3.append(copy)
    for h in range(n_heads):
        for s in range(seqs):
            i = h * seqs + s
            state[s, h] = (
                state[s, h] * decay[s:s + 1, h:h + 1]
                + cols[:, k0 + i:k0 + i + 1] * delta[i:i + 1, :]
            )
    x3_recv[me] = x3_send[...]
    wo_copy.wait()
    for step in range(1, n_dev):
        source = lax.rem(me + step, n_dev)
        pltpu.make_async_remote_copy(
            x3_send, x3_recv.at[source], s3.at[step], r3.at[source],
            device_id=place(source), device_id_type=MESH,
        ).wait_recv()
    heads_f32[...] = x3_recv[...].astype(F32).reshape(heads_f32.shape)
    for t in range(n_tp):
        for h in range(n_heads):
            for s in range(seqs):
                left[t * n_heads + h, pl.ds(s, n_kv, stride=seqs), :] = heads_f32[
                    pl.ds(t * stride3 + h * seqs + s, n_kv, stride=n_tp * stride3), :
                ]
    mixed = None
    for t in range(n_tp):
        lhs = jnp.concatenate(
            [left[t * n_heads + h].astype(BF16) for h in range(n_heads)], axis=1
        )
        half = jnp.dot(lhs, wo[t], preferred_element_type=F32).astype(BF16).astype(F32)
        mixed = half if mixed is None else mixed + half
    resid = (own + mixed).astype(BF16)
    x5_send[...] = resid

    sent5 = []
    for step in far_devices + [0]:
        peer = lax.rem(kv * n_tp + step, n_dev) if step else partner
        copy = pltpu.make_async_remote_copy(
            x5_send, x5_recv.at[me], s5.at[step], r5.at[me],
            device_id=place(peer), device_id_type=MESH,
        )
        copy.start()
        sent5.append(copy)
    x5_recv[me] = resid
    copies[12].wait()

    def arrived5(source):
        pltpu.make_async_remote_copy(
            x5_send, x5_recv.at[source], s5.at[0], r5.at[source],
            device_id=place(source), device_id_type=MESH,
        ).wait_recv()

    up_rows = None
    square2 = None
    for step in [0] + far_first[::-1]:
        chip = lax.rem(kv + step, n_kv)
        if step == 0:
            arrived5(kv * n_tp + other)
        else:
            for t in range(n_tp):
                arrived5(chip * n_tp + t)
        blocks = []
        for t in range(n_tp):
            block = x5_recv[chip * n_tp + t].astype(F32)
            gain = x3_recv[chip * n_tp + t].astype(F32)[items:items + 1, :]
            square2 = block * block if square2 is None else square2 + block * block
            blocks.append((block * gain).astype(BF16))
        deep = n_tp * LANES
        term = jnp.dot(
            jnp.concatenate(blocks, axis=1),
            wup[pl.ds(pl.multiple_of(chip * deep, deep), deep), :],
            preferred_element_type=F32,
        )
        up_rows = term if up_rows is None else up_rows + term
    inverse2 = lax.rsqrt(jnp.sum(square2, axis=1, keepdims=True) / d_model + 1e-06)
    act = jnp.square(jnp.maximum(up_rows * inverse2, 0.0)).astype(BF16)

    copies[13].wait()
    sent6 = []
    own_sum = None
    for step in far_first + [n_kv]:
        chip = lax.rem(kv + step, n_kv)
        deep = n_tp * LANES
        piece = jnp.dot(
            act, wdn[:, pl.ds(pl.multiple_of(chip * deep, deep), deep)], preferred_element_type=F32
        )
        for t in range(n_tp):
            x6_send[chip * n_tp + t] = piece[:, t * LANES:(t + 1) * LANES].astype(BF16)
        if step < n_kv:
            for t in range(n_tp):
                copy = pltpu.make_async_remote_copy(
                    x6_send.at[chip * n_tp + t], x6_recv.at[me],
                    s6.at[step * n_tp + t], r6.at[me],
                    device_id={"kv": chip, "tp": t}, device_id_type=MESH,
                )
                copy.start()
                sent6.append(copy)
        else:
            copy = pltpu.make_async_remote_copy(
                x6_send.at[chip * n_tp + other], x6_recv.at[me],
                s6.at[0], r6.at[me], device_id={"tp": other}, device_id_type=MESH,
            )
            copy.start()
            sent6.append(copy)
            own_sum = jnp.where(first, piece[:, 0:LANES], piece[:, LANES:2 * LANES])
    summed = resid.astype(F32) + own_sum
    for step in range(1, n_dev):
        source = lax.rem(me + step, n_dev)
        pltpu.make_async_remote_copy(
            x6_send.at[source], x6_recv.at[source], s6.at[0], r6.at[source],
            device_id=place(source), device_id_type=MESH,
        ).wait_recv()
        summed = summed + x6_recv[source].astype(F32)
    out_ref[...] = summed.astype(BF16)
    for copy in sent2 + sent3 + sent5 + sent6:
        copy.wait_send()


def fused(n_kv, n_tp, *args):
    (tokens, state, mix_gain, w_query, w_key, w_value, w_beta, w_decay, decay_log, head_gain,
     w_out, ff_gain, w_up, w_down) = args
    batch = tokens.shape[0]
    seqs, n_heads = state.shape[:2]
    items = seqs * n_heads
    n_dev = n_kv * n_tp
    chunks = 3 * n_heads + 2
    stride2 = -(-chunks * seqs // 16) * 16
    stride3 = -(-(items + 1) // 16) * 16
    wide = w_query.shape[1]
    operands = (
        tokens, state, mix_gain[None, :], w_query, w_key, w_value, w_beta.T, w_decay.T,
        decay_log[None, :], head_gain[None, :], w_out, ff_gain[None, :], w_up, w_down,
    )
    operands = [pltpu.with_memory_space_constraint(x, pltpu.HBM) for x in operands]
    dma = pltpu.SemaphoreType.DMA
    vmem = pltpu.VMEM
    scratch = [
        vmem(tokens.shape, BF16), vmem((1, LANES), BF16),
        vmem((w_query.shape[0], 3 * wide), BF16), vmem(w_beta.shape[::-1], BF16),
        vmem(w_decay.shape[::-1], BF16), vmem((1, n_heads), F32), vmem((1, LANES), BF16),
        vmem((n_tp, w_out.shape[0], LANES), BF16), vmem((1, LANES), BF16),
        vmem(w_up.shape, BF16), vmem(w_down.shape, BF16),
        vmem((batch + 8, LANES), BF16), vmem((batch + 8, LANES), BF16),
        vmem((chunks, batch, LANES), F32), vmem((n_kv * stride2, LANES), F32),
        vmem((n_kv, stride2, LANES), BF16), vmem((n_kv, stride2, LANES), BF16),
        vmem((stride3, LANES), BF16), vmem((n_dev, stride3, LANES), BF16),
        vmem((n_dev * stride3, LANES), F32), vmem((n_tp * n_heads, batch, LANES), F32),
        vmem((batch, LANES), BF16), vmem((n_dev, batch, LANES), BF16),
        vmem((n_dev, batch, LANES), BF16), vmem((n_dev, batch, LANES), BF16),
        dma((14,)), dma((2,)), dma((2,)),
        dma((n_kv,)), dma((n_kv,)), dma((n_dev,)), dma((n_dev,)),
        dma((n_dev,)), dma((n_dev,)), dma((n_dev,)), dma((n_dev,)),
    ]
    return pl.pallas_call(
        functools.partial(fused_kernel, n_kv, n_tp),
        out_shape=(
            pltpu.VMEM(tokens.shape, BF16), pltpu.VMEM(state.shape, F32),
        ),
        in_specs=[pl.BlockSpec(memory_space=pltpu.HBM)] * len(operands),
        out_specs=(pl.BlockSpec(memory_space=pltpu.VMEM), pl.BlockSpec(memory_space=pltpu.VMEM)),
        scratch_shapes=scratch,
        compiler_params=pltpu.CompilerParams(
            collective_id=0, has_side_effects=True, vmem_limit_bytes=67043328 - 786432 - 16384
        ),
    )(*operands)


def block_of(n_kv, n_tp, *args):
    tokens, state = args[:2]
    fits = (
        tokens.shape[1] == LANES and n_kv == 8 and n_tp == 2
        and state.shape[3] == LANES and tokens.shape[0] % 8 == 0
    )
    return fused(n_kv, n_tp, *args) if fits else local(*args)


def solution(mesh):
    placed = (
        P("dp", ("kv", "tp")),
        P(("dp", "kv"), "tp", None, None),
        P(("kv", "tp")),
        P("kv", "tp"),
        P("kv", "tp"),
        P("kv", "tp"),
        P("kv", "tp"),
        P("kv", "tp"),
        P("tp"),
        P(),
        P("tp", "kv"),
        P(("kv", "tp")),
        P(None, ("kv", "tp")),
        P(("kv", "tp"), None),
    )
    return jax.shard_map(
        functools.partial(block_of, mesh.shape["kv"], mesh.shape["tp"]),
        mesh=mesh,
        in_specs=placed,
        out_specs=(P("dp", ("kv", "tp")), P(("dp", "kv"), "tp", None, None)),
        check_vma=False,
    )
```

```python
import functools

import jax
import jax.numpy as jnp
from jax import lax
from jax.experimental import pallas as pl
from jax.experimental.pallas import tpu as pltpu
from jax.sharding import PartitionSpec as P

D = 2048


def local(
    tokens,
    state,
    mix_gain,
    w_query,
    w_key,
    w_value,
    w_beta,
    w_decay,
    decay_log,
    head_gain,
    w_out,
    ff_gain,
    w_up,
    w_down,
):
    seq_count = state.shape[0]
    heads_local = state.shape[1]
    head_size = state.shape[2]
    tokens_wide, gain_wide = (
        lax.all_gather(tokens, "tp", axis=1, tiled=True),
        lax.all_gather(mix_gain[None, :], "tp", axis=1, tiled=True),
    )
    wide_float = tokens_wide.astype(jnp.float32)
    scaled = (wide_float * gain_wide.astype(jnp.float32)).astype(jnp.bfloat16)
    query_part = jnp.dot(scaled, w_query, preferred_element_type=jnp.float32)
    key_part = jnp.dot(scaled, w_key, preferred_element_type=jnp.float32)
    value_part = jnp.dot(scaled, w_value, preferred_element_type=jnp.float32)
    gate_part = jnp.concatenate(
        [
            jnp.dot(scaled, w_beta, preferred_element_type=jnp.float32),
            jnp.dot(scaled, w_decay, preferred_element_type=jnp.float32),
        ],
        axis=1,
    )
    square_part = jnp.sum(wide_float * wide_float, axis=1)
    query_sum, key_sum, value_sum, gate_sum, square_sum = (
        lax.psum_scatter(query_part, "kv", scatter_dimension=0, tiled=True),
        lax.psum_scatter(key_part, "kv", scatter_dimension=0, tiled=True),
        lax.psum_scatter(value_part, "kv", scatter_dimension=0, tiled=True),
        lax.psum_scatter(gate_part, "kv", scatter_dimension=0, tiled=True),
        lax.psum_scatter(square_part, "kv", scatter_dimension=0, tiled=True),
    )
    inverse = lax.rsqrt(square_sum / D + 1e-06)[:, None]
    query = (inverse * query_sum).reshape(seq_count, heads_local, head_size)
    key_rows = (inverse * key_sum).reshape(seq_count, heads_local, head_size)
    value = (inverse * value_sum).reshape(seq_count, heads_local, head_size)
    gates = inverse * gate_sum
    beta = jax.nn.sigmoid(gates[:, :heads_local])
    decay = -jnp.exp(decay_log)[None, :] * jax.nn.softplus(gates[:, heads_local:])
    qnorm = query * lax.rsqrt(jnp.sum(query * query, axis=-1, keepdims=True) + 1e-06)
    knorm = key_rows * lax.rsqrt(jnp.sum(key_rows * key_rows, axis=-1, keepdims=True) + 1e-06)
    kept = state * jnp.exp(decay)[:, :, None, None]
    predicted = jnp.sum(kept * knorm[:, :, :, None], axis=2)
    new_state = (
        kept + (beta[:, :, None] * knorm)[:, :, :, None] * (value - predicted)[:, :, None, :]
    )
    heads = jnp.sum(new_state * qnorm[:, :, :, None], axis=2) / jnp.sqrt(jnp.float32(head_size))
    normed = (
        heads
        * lax.rsqrt(jnp.mean(heads * heads, axis=-1, keepdims=True) + 1e-06)
        * head_gain.astype(jnp.float32)
    )
    normed = normed.astype(jnp.bfloat16).reshape(seq_count, heads_local * head_size)
    partial_mix = jnp.dot(
        lax.all_gather(normed, "kv", axis=0, tiled=True), w_out, preferred_element_type=jnp.float32
    )
    mixed = lax.psum_scatter(
        partial_mix.astype(jnp.bfloat16), "tp", scatter_dimension=1, tiled=True
    ).astype(jnp.float32)
    resid = (tokens.astype(jnp.float32) + mixed).astype(jnp.bfloat16)
    resid_float = resid.astype(jnp.float32)
    whole_rows = lax.all_gather(resid, ("kv", "tp"), axis=1, tiled=True)
    whole_gain = lax.all_gather(ff_gain[None, :], ("kv", "tp"), axis=1, tiled=True)
    whole_float = whole_rows.astype(jnp.float32)
    inverse2 = lax.rsqrt(jnp.mean(whole_float * whole_float, axis=1, keepdims=True) + 1e-06)
    scaled2 = (whole_float * whole_gain.astype(jnp.float32)).astype(jnp.bfloat16)
    up_rows = jnp.dot(scaled2, w_up, preferred_element_type=jnp.float32) * inverse2
    act = jnp.square(jax.nn.relu(up_rows)).astype(jnp.bfloat16)
    summed = lax.psum_scatter(
        lax.dot_general(w_down, act, (((0,), (1,)), ((), ())), preferred_element_type=jnp.float32),
        ("kv", "tp"),
        scatter_dimension=0,
        tiled=True,
    )
    results = (resid_float + summed.T).astype(jnp.bfloat16)
    return (results, new_state)


LANES = 128
MESH = pl.DeviceIdType.MESH
F32 = jnp.float32
BF16 = jnp.bfloat16


def fused_kernel(
    n_kv,
    n_tp,
    tok_hbm, state_hbm, mg_hbm, wq_hbm, wk_hbm, wv_hbm, wb_hbm, wd_hbm, dl_hbm, hg_hbm,
    wo_hbm, fg_hbm, wup_hbm, wdn_hbm,
    out_ref, state,
    tok, mg, wqkv, wb, wd, dl, hg, wo, fg, wup, wdn,
    x1_send, x1_recv, parts, rows, x2_send, x2_recv,
    x3_send, x3_recv, heads_f32, left,
    x5_send, x5_recv, x6_send, x6_recv,
    load_sem, go_sem, x1_sems, wo_sems, s2, r2, s3, r3, s5, r5, s6, r6,
):
    kv = lax.axis_index("kv")
    tp = lax.axis_index("tp")
    other = 1 - tp
    n_dev = n_kv * n_tp
    me = kv * n_tp + tp
    batch = tok.shape[0]
    seqs, n_heads, size = state.shape[0], state.shape[1], state.shape[2]
    wide = n_heads * size
    d_model = n_dev * LANES
    items = n_heads * seqs
    stride2 = x2_send.shape[1]
    stride3 = x3_recv.shape[1]

    far_first = sorted(range(1, n_kv), key=lambda step: -min(step, n_kv - step))
    far_devices = [step * n_tp + t for step in far_first for t in range(n_tp)]
    partner = kv * n_tp + other

    def place(device):
        return {"kv": device // n_tp, "tp": lax.rem(device, n_tp)}

    loads = [
        (tok_hbm, tok), (mg_hbm, mg),
        (wq_hbm, wqkv.at[:, 0:wide]),
        (wk_hbm, wqkv.at[:, wide:2 * wide]),
        (wv_hbm, wqkv.at[:, 2 * wide:3 * wide]),
        (wb_hbm, wb), (wd_hbm, wd), (dl_hbm, dl), (hg_hbm, hg), (fg_hbm, fg),
        (wo_hbm.at[:, pl.ds(pl.multiple_of(tp * LANES, LANES), LANES)], wo.at[tp]),
        (state_hbm, state), (wup_hbm, wup), (wdn_hbm, wdn),
    ]
    copies = [
        pltpu.make_async_copy(a, b, load_sem.at[i]) for i, (a, b) in enumerate(loads)
    ]
    for copy in copies:
        copy.start()

    barrier = pltpu.get_barrier_semaphore()
    lead = n_tp - 1
    leads = tp == lead

    @pl.when(leads)
    def _():
        pl.semaphore_signal(barrier, inc=1, device_id={"tp": other}, device_id_type=MESH)

    for step in far_first:
        pl.semaphore_signal(
            barrier, inc=1, device_id={"kv": lax.rem(kv + step, n_kv), "tp": lead},
            device_id_type=MESH,
        )
    rows[...] = jnp.zeros_like(rows)
    copies[0].wait()
    copies[1].wait()
    own = tok[...].astype(F32)
    own_gain = mg[...].astype(F32)
    x1_send[0:batch, :] = tok[...]
    x1_send[batch:, :] = jnp.broadcast_to(own_gain, (x1_send.shape[0] - batch, LANES)).astype(BF16)

    x1 = pltpu.make_async_remote_copy(
        x1_send, x1_recv, x1_sems.at[0], x1_sems.at[1], device_id={"tp": other}, device_id_type=MESH
    )

    @pl.when(jnp.logical_not(leads))
    def _():
        pl.semaphore_wait(barrier, 1)

    @pl.when(leads)
    def _():
        x1.wait_recv()

    x1.start()
    wo_copy = pltpu.make_async_remote_copy(
        wo_hbm.at[:, pl.ds(pl.multiple_of(other * LANES, LANES), LANES)],
        wo.at[tp], wo_sems.at[0], wo_sems.at[1], device_id={"tp": other}, device_id_type=MESH,
    )
    wo_copy.start()
    for copy in copies[2:7]:
        copy.wait()
    low = LANES // 2
    gate_w = jnp.concatenate(
        [
            wb[...].astype(F32), wd[...].astype(F32), jnp.zeros((low - 2 * n_heads, wb.shape[1]), F32),
            wb[...].astype(F32), wd[...].astype(F32),
            jnp.zeros((LANES - low - 2 * n_heads, wb.shape[1]), F32),
        ],
        axis=0,
    ).astype(BF16)
    own_scaled = own * own_gain

    @pl.when(jnp.logical_not(leads))
    def _():
        x1.wait_recv()

    far = x1_recv[0:batch, :].astype(F32)
    far_scaled = far * x1_recv[batch:, :].astype(F32)[0:1, :]
    first = tp == 0
    scaled = jnp.concatenate(
        [jnp.where(first, own_scaled, far_scaled), jnp.where(first, far_scaled, own_scaled)], axis=1
    ).astype(BF16)
    squares = jnp.sum(own * own + far * far, axis=1, keepdims=True)
    gates = lax.dot_general(
        scaled, gate_w, (((1,), (1,)), ((), ())), preferred_element_type=F32
    )
    lane = lax.broadcasted_iota(jnp.int32, gates.shape, 1)
    gates = jnp.where(lax.rem(lane, low) == 2 * n_heads, squares, gates)
    gates_hi = gates.astype(BF16).astype(F32)
    chunks = 3 * n_heads
    product = jnp.dot(scaled, wqkv[...], preferred_element_type=F32)
    for c in range(chunks):
        parts[c] = product[:, c * LANES:(c + 1) * LANES]
    parts[chunks] = jnp.where(lane < low, gates_hi, gates - gates_hi)
    for c in range(chunks + 1):
        for s in range(seqs):
            rows[pl.ds(c * seqs + s, n_kv, stride=stride2), :] = parts[
                c, pl.ds(s, n_kv, stride=seqs), :
            ]
    x2_send[...] = rows[...].reshape(x2_send.shape).astype(BF16)

    @pl.when(leads)
    def _():
        pl.semaphore_wait(barrier, n_dev - n_tp)
        pl.semaphore_signal(go_sem, inc=1, device_id={"tp": other}, device_id_type=MESH)

    @pl.when(jnp.logical_not(leads))
    def _():
        pl.semaphore_wait(go_sem, 1)

    sent2 = []
    for step in far_first:
        peer = lax.rem(kv + step, n_kv)
        copy = pltpu.make_async_remote_copy(
            x2_send.at[peer], x2_recv.at[kv], s2.at[step], r2.at[kv],
            device_id={"kv": peer}, device_id_type=MESH,
        )
        copy.start()
        sent2.append(copy)
    x2_recv[kv] = x2_send[kv]
    for copy in copies[7:12]:
        copy.wait()
    for step in range(1, n_kv):
        source = lax.rem(kv + step, n_kv)
        pltpu.make_async_remote_copy(
            x2_send.at[source], x2_recv.at[source], s2.at[step], r2.at[source],
            device_id={"kv": source}, device_id_type=MESH,
        ).wait_recv()
    total = x2_recv[0].astype(F32)
    for k in range(1, n_kv):
        total = total + x2_recv[k].astype(F32)

    g0 = 3 * items
    gate = total[g0:g0 + seqs, :]
    gate = gate[:, 0:low] + gate[:, low:]
    inverse = lax.rsqrt(gate[:, 2 * n_heads:2 * n_heads + 1] / d_model + 1e-06)
    gate = gate * inverse
    beta = jax.nn.sigmoid(gate[:, 0:n_heads])
    decay = jnp.exp(-jnp.exp(dl[...]) * jax.nn.softplus(gate[:, n_heads:2 * n_heads]))
    inv_col = jnp.concatenate([inverse] * n_heads, axis=0)
    query = total[0:items, :] * inv_col
    key_rows = total[items:2 * items, :] * inv_col
    value = total[2 * items:3 * items, :] * inv_col
    qnorm = query * lax.rsqrt(jnp.sum(query * query, axis=1, keepdims=True) + 1e-06)
    knorm = key_rows * lax.rsqrt(jnp.sum(key_rows * key_rows, axis=1, keepdims=True) + 1e-06)
    fill = jnp.zeros((-items % 8, LANES), F32)
    cols = jnp.transpose(jnp.concatenate([qnorm, fill, knorm, fill], axis=0))
    k0 = items + fill.shape[0]
    along_k, along_q = [], []
    for h in range(n_heads):
        for s in range(seqs):
            i = h * seqs + s
            before = state[s, h]
            along_k.append(jnp.sum(before * cols[:, k0 + i:k0 + i + 1], axis=0, keepdims=True))
            along_q.append(jnp.sum(before * cols[:, i:i + 1], axis=0, keepdims=True))
    beta_col = jnp.concatenate([beta[:, h:h + 1] for h in range(n_heads)], axis=0)
    decay_col = jnp.concatenate([decay[:, h:h + 1] for h in range(n_heads)], axis=0)
    delta = beta_col * (value - decay_col * jnp.concatenate(along_k, axis=0))
    heads = (
        decay_col * jnp.concatenate(along_q, axis=0)
        + jnp.sum(qnorm * knorm, axis=1, keepdims=True) * delta
    ) / jnp.sqrt(F32(size))
    normed = (
        heads * lax.rsqrt(jnp.mean(heads * heads, axis=1, keepdims=True) + 1e-06)
        * hg[...].astype(F32)
    )
    x3_send[...] = jnp.concatenate(
        [normed, jnp.broadcast_to(fg[...].astype(F32), (stride3 - items, LANES))], axis=0
    ).astype(BF16)

    sent3 = []
    for step in far_devices + [0]:
        peer = lax.rem(kv * n_tp + step, n_dev) if step else partner
        copy = pltpu.make_async_remote_copy(
            x3_send, x3_recv.at[me], s3.at[step], r3.at[me],
            device_id=place(peer), device_id_type=MESH,
        )
        copy.start()
        sent3.append(copy)
    for h in range(n_heads):
        for s in range(seqs):
            i = h * seqs + s
            state[s, h] = (
                state[s, h] * decay[s:s + 1, h:h + 1]
                + cols[:, k0 + i:k0 + i + 1] * delta[i:i + 1, :]
            )
    x3_recv[me] = x3_send[...]
    wo_copy.wait()
    for step in range(1, n_dev):
        source = lax.rem(me + step, n_dev)
        pltpu.make_async_remote_copy(
            x3_send, x3_recv.at[source], s3.at[step], r3.at[source],
            device_id=place(source), device_id_type=MESH,
        ).wait_recv()
    heads_f32[...] = x3_recv[...].astype(F32).reshape(heads_f32.shape)
    for t in range(n_tp):
        for h in range(n_heads):
            for s in range(seqs):
                left[t * n_heads + h, pl.ds(s, n_kv, stride=seqs), :] = heads_f32[
                    pl.ds(t * stride3 + h * seqs + s, n_kv, stride=n_tp * stride3), :
                ]
    mixed = None
    for t in range(n_tp):
        lhs = jnp.concatenate(
            [left[t * n_heads + h].astype(BF16) for h in range(n_heads)], axis=1
        )
        half = jnp.dot(lhs, wo[t], preferred_element_type=F32).astype(BF16).astype(F32)
        mixed = half if mixed is None else mixed + half
    resid = (own + mixed).astype(BF16)
    x5_send[...] = resid

    sent5 = []
    for step in far_devices + [0]:
        peer = lax.rem(kv * n_tp + step, n_dev) if step else partner
        copy = pltpu.make_async_remote_copy(
            x5_send, x5_recv.at[me], s5.at[step], r5.at[me],
            device_id=place(peer), device_id_type=MESH,
        )
        copy.start()
        sent5.append(copy)
    x5_recv[me] = resid
    copies[12].wait()

    def arrived5(source):
        pltpu.make_async_remote_copy(
            x5_send, x5_recv.at[source], s5.at[0], r5.at[source],
            device_id=place(source), device_id_type=MESH,
        ).wait_recv()

    up_rows = None
    square2 = None
    for step in [0] + far_first[::-1]:
        chip = lax.rem(kv + step, n_kv)
        if step == 0:
            arrived5(kv * n_tp + other)
        else:
            for t in range(n_tp):
                arrived5(chip * n_tp + t)
        blocks = []
        for t in range(n_tp):
            block = x5_recv[chip * n_tp + t].astype(F32)
            gain = x3_recv[chip * n_tp + t].astype(F32)[items:items + 1, :]
            square2 = block * block if square2 is None else square2 + block * block
            blocks.append((block * gain).astype(BF16))
        deep = n_tp * LANES
        term = jnp.dot(
            jnp.concatenate(blocks, axis=1),
            wup[pl.ds(pl.multiple_of(chip * deep, deep), deep), :],
            preferred_element_type=F32,
        )
        up_rows = term if up_rows is None else up_rows + term
    inverse2 = lax.rsqrt(jnp.sum(square2, axis=1, keepdims=True) / d_model + 1e-06)
    act = jnp.square(jnp.maximum(up_rows * inverse2, 0.0)).astype(BF16)

    copies[13].wait()
    sent6 = []
    own_sum = None
    for step in far_first + [n_kv]:
        chip = lax.rem(kv + step, n_kv)
        deep = n_tp * LANES
        piece = jnp.dot(
            act, wdn[:, pl.ds(pl.multiple_of(chip * deep, deep), deep)], preferred_element_type=F32
        )
        for t in range(n_tp):
            x6_send[chip * n_tp + t] = piece[:, t * LANES:(t + 1) * LANES].astype(BF16)
        if step < n_kv:
            for t in range(n_tp):
                copy = pltpu.make_async_remote_copy(
                    x6_send.at[chip * n_tp + t], x6_recv.at[me],
                    s6.at[step * n_tp + t], r6.at[me],
                    device_id={"kv": chip, "tp": t}, device_id_type=MESH,
                )
                copy.start()
                sent6.append(copy)
        else:
            copy = pltpu.make_async_remote_copy(
                x6_send.at[chip * n_tp + other], x6_recv.at[me],
                s6.at[0], r6.at[me], device_id={"tp": other}, device_id_type=MESH,
            )
            copy.start()
            sent6.append(copy)
            own_sum = jnp.where(first, piece[:, 0:LANES], piece[:, LANES:2 * LANES])
    summed = resid.astype(F32) + own_sum
    for step in range(1, n_dev):
        source = lax.rem(me + step, n_dev)
        pltpu.make_async_remote_copy(
            x6_send.at[source], x6_recv.at[source], s6.at[0], r6.at[source],
            device_id=place(source), device_id_type=MESH,
        ).wait_recv()
        summed = summed + x6_recv[source].astype(F32)
    out_ref[...] = summed.astype(BF16)
    for copy in [x1] + sent2 + sent3 + sent5 + sent6:
        copy.wait_send()


def store_kernel(out_ref, state_ref, out_hbm, state_hbm, sems):
    pieces = [(out_ref, out_hbm)] + [
        (state_ref.at[s, h], state_hbm.at[s, h])
        for s in range(state_ref.shape[0])
        for h in range(state_ref.shape[1])
    ]
    copies = [
        pltpu.make_async_copy(a, b, sems.at[i]) for i, (a, b) in enumerate(pieces)
    ]
    for copy in copies:
        copy.start()
    for copy in copies:
        copy.wait()


def store_results(output, state):
    return pl.pallas_call(
        store_kernel,
        out_shape=(
            jax.ShapeDtypeStruct(output.shape, output.dtype),
            jax.ShapeDtypeStruct(state.shape, state.dtype),
        ),
        in_specs=[pl.BlockSpec(memory_space=pltpu.VMEM)] * 2,
        out_specs=(pl.BlockSpec(memory_space=pl.ANY),) * 2,
        scratch_shapes=[pltpu.SemaphoreType.DMA((1 + state.shape[0] * state.shape[1],))],
        compiler_params=pltpu.CompilerParams(vmem_limit_bytes=1024 * 1024),
    )(output, state)


def fused(n_kv, n_tp, *args):
    (tokens, state, mix_gain, w_query, w_key, w_value, w_beta, w_decay, decay_log, head_gain,
     w_out, ff_gain, w_up, w_down) = args
    batch = tokens.shape[0]
    seqs, n_heads = state.shape[:2]
    items = seqs * n_heads
    n_dev = n_kv * n_tp
    chunks = 3 * n_heads + 1
    stride2 = -(-chunks * seqs // 8) * 8
    stride3 = -(-(items + 1) // 16) * 16
    wide = w_query.shape[1]
    operands = (
        tokens, state, mix_gain[None, :], w_query, w_key, w_value, w_beta.T, w_decay.T,
        decay_log[None, :], head_gain[None, :], w_out, ff_gain[None, :], w_up, w_down,
    )
    operands = [pltpu.with_memory_space_constraint(x, pltpu.HBM) for x in operands]
    dma = pltpu.SemaphoreType.DMA
    vmem = pltpu.VMEM
    scratch = [
        vmem(tokens.shape, BF16), vmem((1, LANES), BF16),
        vmem((w_query.shape[0], 3 * wide), BF16), vmem(w_beta.shape[::-1], BF16),
        vmem(w_decay.shape[::-1], BF16), vmem((1, n_heads), F32), vmem((1, LANES), BF16),
        vmem((n_tp, w_out.shape[0], LANES), BF16), vmem((1, LANES), BF16),
        vmem(w_up.shape, BF16), vmem(w_down.shape, BF16),
        vmem((batch + 8, LANES), BF16), vmem((batch + 8, LANES), BF16),
        vmem((chunks, batch, LANES), F32), vmem((n_kv * stride2, LANES), F32),
        vmem((n_kv, stride2, LANES), BF16), vmem((n_kv, stride2, LANES), BF16),
        vmem((stride3, LANES), BF16), vmem((n_dev, stride3, LANES), BF16),
        vmem((n_dev * stride3, LANES), F32), vmem((n_tp * n_heads, batch, LANES), F32),
        vmem((batch, LANES), BF16), vmem((n_dev, batch, LANES), BF16),
        vmem((n_dev, batch, LANES), BF16), vmem((n_dev, batch, LANES), BF16),
        dma((14,)), pltpu.SemaphoreType.REGULAR, dma((2,)), dma((2,)),
        dma((n_kv,)), dma((n_kv,)), dma((n_dev,)), dma((n_dev,)),
        dma((n_dev,)), dma((n_dev,)), dma((n_dev,)), dma((n_dev,)),
    ]
    results = pl.pallas_call(
        functools.partial(fused_kernel, n_kv, n_tp),
        out_shape=(
            pltpu.VMEM(tokens.shape, BF16), pltpu.VMEM(state.shape, F32),
        ),
        in_specs=[pl.BlockSpec(memory_space=pltpu.HBM)] * len(operands),
        out_specs=(pl.BlockSpec(memory_space=pltpu.VMEM), pl.BlockSpec(memory_space=pltpu.VMEM)),
        scratch_shapes=scratch,
        compiler_params=pltpu.CompilerParams(
            collective_id=0, has_side_effects=True, vmem_limit_bytes=67043328 - 786432 - 16384
        ),
    )(*operands)
    return store_results(*results)


def block_of(n_kv, n_tp, *args):
    tokens, state = args[:2]
    fits = (
        tokens.shape[1] == LANES and n_kv == 8 and n_tp == 2
        and state.shape[3] == LANES and tokens.shape[0] % 8 == 0
    )
    return fused(n_kv, n_tp, *args) if fits else local(*args)


def solution(mesh):
    placed = (
        P("dp", ("kv", "tp")),
        P(("dp", "kv"), "tp", None, None),
        P(("kv", "tp")),
        P("kv", "tp"),
        P("kv", "tp"),
        P("kv", "tp"),
        P("kv", "tp"),
        P("kv", "tp"),
        P("tp"),
        P(),
        P("tp", "kv"),
        P(("kv", "tp")),
        P(None, ("kv", "tp")),
        P(("kv", "tp"), None),
    )
    return jax.shard_map(
        functools.partial(block_of, mesh.shape["kv"], mesh.shape["tp"]),
        mesh=mesh,
        in_specs=placed,
        out_specs=(P("dp", ("kv", "tp")), P(("dp", "kv"), "tp", None, None)),
        check_vma=False,
    )
```
